32 devices in a mesh: grp: 2 (over y), sp: 4 (over z), tp: 4 (over x, core).
Axes of the slice: x: 2, y: 2, z: 4, core: 2. Of those that a mesh axis runs over, the one named last changes fastest.
Arguments:
- tokens: bfloat16 [3072, 2048], P(('grp', 'sp')), parts along dimension 0, may hold values from -6 to 6
- norm_gain: float32 [2, 2048], replicated, may hold values from 0.1 to 1.9
- entry_weight: bfloat16 [2, 2048, 2048], P(None, 'sp', 'tp'), may hold values from -0.125 to 0.125
- mix_weight: bfloat16 [2, 4, 512, 512], P(None, 'tp'), may hold values from -0.25 to 0.25
- pool_gain: float32 [2, 2048], P(None, 'tp'), may hold values from 0.1 to 1.9
- back_weight: bfloat16 [2, 2048, 2048], P(None, 'tp', 'sp'), may hold values from -0.25 to 0.25
Outputs:
- result_tokens: bfloat16 [3072, 2048], P(('grp', 'sp')), parts along dimension 0
The draws below stay inside these ranges and needn't reach their ends.
There are 2 independent parts, one for each index of `grp`. The reference program is written for one: setup_inputs(seed, part) draws one part's arguments, and reference() takes and returns one part's arrays. A program takes and returns all parts, laid end to end along the dimension named above; an argument that names none is the same for every part. Nothing has to cross between parts.
All inputs are finite; a program needn't handle non-finite values.
Results may differ from the reference program's by a relative error of at most 0.018.
Values may be sent and summed in bfloat16 or wider, within the bound.
A program may use at most 64 MiB of HBM per device.

```python
import jax
import jax.numpy as jnp
from jax import lax

D = 2048
GROUPS = 4
POOL_W = 2048
GROUP_W = 512
LAYERS = 2
LENGTH = 1536
N_TP = 4


def steps_of(own_key, extent, shards, low, largest):
    factor_of = 1.0
    for axis_at, parts in shards:
        heights = jax.random.uniform(jax.random.fold_in(jax.random.fold_in(own_key, 6), axis_at), (parts,), jnp.float32, low / len(shards), largest / len(shards))
        factor_of = factor_of * jnp.repeat(jnp.exp(heights), extent[axis_at] // parts).reshape((-1,) + (1,) * (len(extent) - 1 - axis_at))
    return factor_of


def normal_values(stream_key, dims, width, bound, split=(), held_as=jnp.bfloat16):
    values = jax.random.normal(stream_key, dims, jnp.float32) * width
    if len(split) > 0:
        values = steps_of(stream_key, dims, split, -0.22, 0.18) * values
    return jnp.clip(values, min=-bound, max=bound).astype(held_as)


def setup_inputs(seed: int = 0, part: int = 0) -> dict:
    splits = jax.random.split(jax.random.key(seed), 7)
    part_splits = jax.random.split(jax.random.fold_in(splits[6], part), 7)
    return {
        "tokens": normal_values(part_splits[0], (LENGTH, D), 1.0, 6.0, ((0, 4),)),
        "norm_gain": jnp.clip(1.0 + 0.18 * jax.random.normal(splits[1], (LAYERS, D), jnp.float32), 0.1, 1.9),
        "entry_weight": normal_values(splits[2], (LAYERS, D, POOL_W), D ** -0.5, 0.125, ((1, 4), (2, 4))),
        "mix_weight": normal_values(splits[3], (LAYERS, GROUPS, GROUP_W, GROUP_W), GROUP_W ** -0.5, 0.25, ((1, 4),)),
        "pool_gain": jnp.clip(1.0 + 0.18 * jax.random.normal(splits[4], (LAYERS, POOL_W), jnp.float32), 0.1, 1.9),
        "back_weight": normal_values(splits[5], (LAYERS, POOL_W, D), (POOL_W // 4) ** -0.5, 0.25, ((1, 4), (2, 4))),
    }


EPSILON = 1e-05

def window_mean(padded, positions, halves, total_length, reach):
    row_count = positions.shape[0]
    summed = jnp.zeros((row_count,) + padded.shape[1:], jnp.float32)
    for offset in range(-reach, reach):
        inside = ((offset >= -halves) & (offset < halves)).astype(jnp.float32)
        summed = summed + padded[reach + offset:reach + offset + row_count] * inside[None, :, None]
    lower = jnp.maximum(positions[:, None] - halves[None, :], 0)
    upper = jnp.minimum(positions[:, None] + halves[None, :], total_length)
    counted = (upper - lower).astype(jnp.float32)
    return summed / counted[:, :, None]

def reference(tokens, norm_gain, entry_weight, mix_weight, pool_gain, back_weight):
    reach = 2 ** (GROUPS - 1)
    halves = jnp.left_shift(jnp.int32(1), jnp.arange(GROUPS, dtype=jnp.int32))
    positions = jnp.arange(LENGTH, dtype=jnp.int32)
    block_width = POOL_W // N_TP
    state = tokens
    for layer in range(LAYERS):
        values = state.astype(jnp.float32)
        scaled = values * lax.rsqrt(lax.optimization_barrier(jnp.mean(values * values, axis=-1, keepdims=True)) + EPSILON)
        normed = (scaled * norm_gain[layer].astype(jnp.float32)).astype(jnp.bfloat16)
        pooled_in = jnp.dot(normed, entry_weight[layer], preferred_element_type=jnp.float32).astype(jnp.bfloat16)
        grouped = pooled_in.reshape(LENGTH, GROUPS, GROUP_W).astype(jnp.float32)
        padded = jnp.pad(grouped, ((reach, reach), (0, 0), (0, 0)))
        means = window_mean(padded, positions, halves, LENGTH, reach)
        differ = (means - grouped).astype(jnp.bfloat16)
        mixed = jnp.einsum('tgc,gcd->tgd', differ.astype(jnp.float32), mix_weight[layer].astype(jnp.float32))
        mixed = (mixed.reshape(LENGTH, POOL_W) * pool_gain[layer].astype(jnp.float32)).astype(jnp.bfloat16)
        total = values
        for block in range(N_TP):
            term = jnp.dot(mixed[:, block * block_width:(block + 1) * block_width], back_weight[layer, block * block_width:(block + 1) * block_width], preferred_element_type=jnp.float32)
            total = total + lax.optimization_barrier(term.astype(jnp.bfloat16)).astype(jnp.float32)
        state = total.astype(jnp.bfloat16)
    return state
```

```python
import functools

import jax
import jax.numpy as jnp
from jax import lax
from jax.experimental import pallas as pl
from jax.experimental.pallas import tpu as pltpu
from jax.sharding import PartitionSpec as P

EPSILON = 1e-05
MESH = pl.DeviceIdType.MESH
LANES = 128
GROUPS = 4
LAYERS = 2
HALO = 16
SUBS = 2


def kernel(
    sizes,
    tok_ref, gain_ref, entry_ref, mix_ref, pgain_ref, back_ref,
    out_ref,
    went, wback, state, normed, ext, mixed, t_own, t_out, t_in, s_own, s_in,
    zsend, zrecv, ysend, yrecv, hsend, hrecv, asend, arecv, bsend, brecv, csend, crecv, lsem,
):
    n_g, n_s, n_t = sizes
    layers, depth, width = entry_ref.shape
    rows, channels = tok_ref.shape
    cols = back_ref.shape[2]
    half = rows // 2
    pairs = 2 if n_g % 2 == 0 else 1
    g, s, t = lax.axis_index("grp"), lax.axis_index("sp"), lax.axis_index("tp")
    h = lax.rem(g, pairs)
    y_dev = {"grp": g + 1 - 2 * h}
    core = lax.rem(t, 2)
    chip = lax.rem(t // 2, 2)
    core_dev = {"tp": t + 1 - 2 * core}
    x_dev = {"tp": t + 2 - 4 * chip}
    right, left = {"sp": s + 1}, {"sp": s - 1}
    has_right, has_left = s < n_s - 1, s > 0

    barrier = pltpu.get_barrier_semaphore()

    def greet(device):
        pl.semaphore_signal(barrier, inc=1, device_id=device, device_id_type=MESH)

    greet(core_dev)
    greet(x_dev)
    if pairs == 2:
        greet(y_dev)
    pl.when(has_right)(lambda: greet(right))
    pl.when(has_left)(lambda: greet(left))
    pl.semaphore_wait(
        barrier, 1 + pairs + has_right.astype(jnp.int32) + has_left.astype(jnp.int32)
    )

    block_rows = (depth, back_ref.shape[1])

    def piece(m, o, part, c):
        layer, which = divmod(m, 2)
        size = block_rows[which] // (pairs * SUBS)
        start = pl.multiple_of((part * SUBS + c) * size, size)
        if which == 0:
            return went.at[layer, pl.ds(pl.multiple_of(o * depth + start, size), size)]
        return wback.at[layer, o, pl.ds(start, size)]

    def own_piece(m, c):
        layer, which = divmod(m, 2)
        size = block_rows[which] // (pairs * SUBS)
        ref = (entry_ref, back_ref)[which]
        return ref.at[layer, pl.ds(pl.multiple_of((h * SUBS + c) * size, size), size)]

    def z_copy(m, o, c, to_right, own=False):
        return pltpu.make_async_remote_copy(
            src_ref=own_piece(m, c) if own else piece(m, o, h, c),
            dst_ref=piece(m, o, h, c),
            send_sem=zsend.at[m, o, c, 0 if to_right else 1],
            recv_sem=zrecv.at[m, o, c],
            device_id=right if to_right else left,
            device_id_type=MESH,
        )

    def y_copy(m, o, c, part):
        return pltpu.make_async_remote_copy(
            src_ref=piece(m, o, part, c),
            dst_ref=piece(m, o, part, c),
            send_sem=ysend.at[m, o, c],
            recv_sem=yrecv.at[m, o, c],
            device_id=y_dev,
            device_id_type=MESH,
        )

    def send_own(m):
        for c in range(SUBS):
            pl.when(has_right)(lambda: z_copy(m, s, c, True, own=True).start())
            pl.when(has_left)(lambda: z_copy(m, s, c, False, own=True).start())

    def sides(d):
        return ((s >= d, s - d, True, has_right), (s + d < n_s, s + d, False, has_left))

    def forward(m, d):
        for c in range(SUBS):
            for there, o, to_right, onward in sides(d):
                @pl.when(there)
                def _():
                    z_copy(m, o, c, to_right).wait_recv()
                    pl.when(onward)(lambda: z_copy(m, o, c, to_right).start())
                    if pairs == 2:
                        y_copy(m, o, c, h).start()

    def await_y(m, o):
        if pairs == 2:
            for c in range(SUBS):
                y_copy(m, o, c, 1 - h).wait_recv()

    def await_y_all(m):
        for d in range(1, n_s):
            for there, o, _, _ in sides(d):
                pl.when(there)(lambda: await_y(m, o))

    send_own(0)

    locals_ = []
    for layer in range(layers):
        locals_.append(
            pltpu.make_async_copy(
                entry_ref.at[layer],
                went.at[layer, pl.ds(pl.multiple_of(s * depth, depth), depth)],
                lsem.at[2 * layer],
            )
        )
        locals_.append(
            pltpu.make_async_copy(back_ref.at[layer], wback.at[layer, s], lsem.at[2 * layer + 1])
        )
    for copy in locals_:
        copy.start()
    for o in range(n_s):
        state[o] = tok_ref[:, o * cols:(o + 1) * cols]

    def normalize(layer):
        def body(i, carry):
            at = pl.ds(pl.multiple_of(i * 32, 32), 32)
            total = jnp.zeros((32, 1), jnp.float32)
            for o in range(n_s):
                value = state[o, at, :].astype(jnp.float32)
                total = total + jnp.sum(value * value, axis=-1, keepdims=True)
            scale = lax.rsqrt(total / channels + EPSILON)
            for o in range(n_s):
                value = state[o, at, :].astype(jnp.float32)
                gain = gain_ref[layer:layer + 1, o * cols:(o + 1) * cols]
                normed[at, o * cols:(o + 1) * cols] = (value * scale * gain).astype(jnp.bfloat16)
            return carry

        lax.fori_loop(0, rows // 32, body, 0)

    def halo_copy(layer, to_right):
        src = rows - HALO if to_right else 0
        dst = rows if to_right else rows + HALO
        side = 0 if to_right else 1
        return pltpu.make_async_remote_copy(
            src_ref=ext.at[layer, pl.ds(src, HALO)],
            dst_ref=ext.at[layer, pl.ds(dst, HALO)],
            send_sem=hsend.at[layer, side],
            recv_sem=hrecv.at[layer, side],
            device_id=right if to_right else left,
            device_id_type=MESH,
        )

    def entry(layer):
        ext[layer, 0:rows] = jnp.dot(
            normed[...], went[layer], preferred_element_type=jnp.float32
        ).astype(jnp.bfloat16)
        pl.when(has_right)(lambda: halo_copy(layer, True).start())
        pl.when(has_left)(lambda: halo_copy(layer, False).start())
        zero = jnp.zeros((HALO, width), jnp.bfloat16)

        @pl.when(s == 0)
        def _():
            ext[layer, rows:rows + HALO] = zero

        @pl.when(s == n_s - 1)
        def _():
            ext[layer, rows + HALO:rows + 2 * HALO] = zero

    def pool(layer):
        pl.when(has_left)(lambda: halo_copy(layer, True).wait_recv())
        pl.when(has_right)(lambda: halo_copy(layer, False).wait_recv())
        reach = jnp.left_shift(jnp.int32(1), t)
        shape = (rows, rows + 2 * HALO)
        row = lax.broadcasted_iota(jnp.int32, shape, 0)
        j = lax.broadcasted_iota(jnp.int32, shape, 1)
        position = jnp.where(j < rows, j, jnp.where(j < rows + HALO, j - rows - HALO, j - HALO))
        offset = position - row
        band = jnp.where((offset >= -reach) & (offset < reach), 1.0, 0.0).astype(jnp.bfloat16)
        summed = jnp.dot(band, ext[layer], preferred_element_type=jnp.float32)
        at = s * rows + lax.broadcasted_iota(jnp.int32, (rows, 1), 0)
        counted = jnp.minimum(at + reach, n_s * rows) - jnp.maximum(at - reach, 0)
        means = summed / counted.astype(jnp.float32)
        differ = (means - ext[layer, 0:rows].astype(jnp.float32)).astype(jnp.bfloat16)
        product = jnp.dot(differ, mix_ref[layer, 0], preferred_element_type=jnp.float32)
        mixed[...] = (product * pgain_ref[layer:layer + 1, :]).astype(jnp.bfloat16)

    keep = pl.ds(pl.multiple_of(core * half, half), half)
    give = pl.ds(pl.multiple_of((1 - core) * half, half), half)
    turn = 1 - 2 * (s // ((n_s + 1) // 2))

    def block_of(k):
        return lax.rem(s + turn * k + n_s, n_s)

    def a_copy(layer, k):
        return pltpu.make_async_remote_copy(
            src_ref=t_out.at[layer, k], dst_ref=t_in.at[layer, k],
            send_sem=asend.at[layer, k], recv_sem=arecv.at[layer, k],
            device_id=core_dev, device_id_type=MESH,
        )

    def b_copy(layer, k):
        return pltpu.make_async_remote_copy(
            src_ref=s_own.at[layer, k], dst_ref=s_in.at[layer, k],
            send_sem=bsend.at[layer, k], recv_sem=brecv.at[layer, k],
            device_id=x_dev, device_id_type=MESH,
        )

    def c_copy(layer, k, rows_at):
        o = block_of(k)
        return pltpu.make_async_remote_copy(
            src_ref=state.at[o, rows_at], dst_ref=state.at[o, rows_at],
            send_sem=csend.at[layer, k], recv_sem=crecv.at[layer, k],
            device_id=core_dev, device_id_type=MESH,
        )

    def back(layer, k):
        o = block_of(k)
        if k > 0:
            await_y(2 * layer + 1, o)
        weight = wback[layer, o]
        t_out[layer, k] = jnp.dot(
            mixed[give, :], weight, preferred_element_type=jnp.float32
        ).astype(jnp.bfloat16)
        a_copy(layer, k).start()
        t_own[...] = jnp.dot(mixed[keep, :], weight, preferred_element_type=jnp.float32).astype(
            jnp.bfloat16
        )
        a_copy(layer, k).wait_recv()
        s_own[layer, k] = (
            t_own[...].astype(jnp.float32) + t_in[layer, k].astype(jnp.float32)
        ).astype(jnp.bfloat16)
        b_copy(layer, k).start()

    def finish(layer, k):
        o = block_of(k)
        b_copy(layer, k).wait_recv()
        state[o, keep] = (
            state[o, keep].astype(jnp.float32)
            + (s_own[layer, k].astype(jnp.float32) + s_in[layer, k].astype(jnp.float32))
        ).astype(jnp.bfloat16)
        c_copy(layer, k, keep).start()

    def settle(layer):
        for k in range(n_s):
            c_copy(layer, k, give).wait_recv()
            c_copy(layer, k, keep).wait_send()

    normalize(0)
    for d in range(1, n_s):
        forward(0, d)
    for layer in range(layers):
        m = 2 * layer
        send_own(m + 1)
        if layer == 0:
            for copy in locals_:
                copy.wait()
        forward(m + 1, 1)
        await_y_all(m)
        entry(layer)
        for d in range(2, n_s - 1):
            forward(m + 1, d)
        pool(layer)
        last = layer == layers - 1
        if last:
            back(layer, 0)
            back(layer, 1)
        for d in range(max(2, n_s - 1), n_s):
            forward(m + 1, d)
        if not last:
            send_own(m + 2)
            back(layer, 0)
            back(layer, 1)
            forward(m + 2, 1)
        for k in range(2, n_s):
            back(layer, k)
        if not last and n_s > 2:
            forward(m + 2, 2)
        for k in range(n_s):
            finish(layer, k)
        if not last:
            for d in range(3, n_s):
                forward(m + 2, d)
        settle(layer)
        if not last:
            normalize(layer + 1)

    for o in range(n_s):
        out_ref[:, o * cols:(o + 1) * cols] = state[o]

    for layer in range(layers):
        pl.when(has_right)(lambda: halo_copy(layer, True).wait_send())
        pl.when(has_left)(lambda: halo_copy(layer, False).wait_send())
        for k in range(n_s):
            a_copy(layer, k).wait_send()
            b_copy(layer, k).wait_send()
    for m in range(2 * layers):
        for c in range(SUBS):
            pl.when(has_right)(lambda: z_copy(m, s, c, True, own=True).wait_send())
            pl.when(has_left)(lambda: z_copy(m, s, c, False, own=True).wait_send())
            for d in range(1, n_s):
                for there, o, to_right, onward in sides(d):
                    @pl.when(there)
                    def _():
                        pl.when(onward)(lambda: z_copy(m, o, c, to_right).wait_send())
                        if pairs == 2:
                            y_copy(m, o, c, h).wait_send()


def extended_2(value, sides, width):
    for axis, dim in sides:
        size, length = (lax.axis_size(axis), value.shape[dim])
        up = [(i, (i + 1) % size) for i in range(size - 1)]
        down = [(j, i) for i, j in up]
        last = lax.slice_in_dim(value, length - width, length, axis=dim)
        first = lax.slice_in_dim(value, 0, width, axis=dim)
        before = lax.ppermute(last, axis, up)
        after = lax.ppermute(first, axis, down)
        value = jnp.concatenate([before, value, after], axis=dim)
    return value


def window_mean(padded, positions, halves, total_length, reach):
    row_count = positions.shape[0]
    summed = jnp.zeros((row_count,) + padded.shape[1:], jnp.float32)
    for offset in range(-reach, reach):
        inside = ((offset >= -halves) & (offset < halves)).astype(jnp.float32)
        summed = (
            summed + padded[reach + offset : reach + offset + row_count] * inside[None, :, None]
        )
    lower = jnp.maximum(positions[:, None] - halves[None, :], 0)
    upper = jnp.minimum(positions[:, None] + halves[None, :], total_length)
    counted = (upper - lower).astype(jnp.float32)
    return summed / counted[:, :, None]


def normalize(state, gain):
    values = state.astype(jnp.float32)
    scaled = values * lax.rsqrt(jnp.mean(values * values, axis=-1, keepdims=True) + EPSILON)
    return (scaled * gain).astype(jnp.bfloat16)


def pool_groups(pooled_in, mix_layer, gain_layer, reach):
    row_count = pooled_in.shape[0]
    group_here = mix_layer.shape[0]
    width = mix_layer.shape[1]
    extended = extended_2(pooled_in, (("sp", 0),), reach)
    first_group = lax.axis_index("tp") * group_here
    halves = jnp.left_shift(jnp.int32(1), first_group + jnp.arange(group_here, dtype=jnp.int32))
    positions = lax.axis_index("sp") * row_count + jnp.arange(row_count, dtype=jnp.int32)
    total_length = lax.axis_size("sp") * row_count
    padded = extended.reshape(row_count + 2 * reach, group_here, width).astype(jnp.float32)
    means = window_mean(padded, positions, halves, total_length, reach)
    differ = (means - padded[reach : reach + row_count]).astype(jnp.bfloat16)
    mixed = jnp.einsum("tgc,gcd->tgd", differ, mix_layer, preferred_element_type=jnp.float32)
    return (mixed.reshape(row_count, group_here * width) * gain_layer).astype(jnp.bfloat16)


def plain(tokens, norm_gain, entry_weight, mix_weight, pool_gain, back_weight):
    reach = 2 ** (GROUPS - 1)
    state = tokens
    entry_all, back_all = (
        lax.all_gather(entry_weight, "sp", axis=1, tiled=True),
        lax.all_gather(back_weight, "sp", axis=2, tiled=True),
    )
    for layer in range(LAYERS):
        normed = normalize(state, norm_gain[layer])
        pooled_in = jnp.dot(normed, entry_all[layer], preferred_element_type=jnp.float32).astype(
            jnp.bfloat16
        )
        back_local = back_all[layer]
        mixed = pool_groups(pooled_in, mix_weight[layer], pool_gain[layer], reach)
        update = jnp.dot(mixed, back_local, preferred_element_type=jnp.float32)
        summed = lax.psum(update.astype(jnp.bfloat16), "tp").astype(jnp.float32)
        state = (state.astype(jnp.float32) + summed).astype(jnp.bfloat16)
    return state


def solution(mesh):
    n_g, n_s, n_t = mesh.shape["grp"], mesh.shape["sp"], mesh.shape["tp"]

    def per_device(tokens, norm_gain, entry_weight, mix_weight, pool_gain, back_weight):
        layers, depth, width = entry_weight.shape
        rows, channels = tokens.shape
        cols = back_weight.shape[2]
        half = rows // 2
        if n_t != 4 or cols % LANES or depth % LANES or rows % (2 * HALO):
            return plain(tokens, norm_gain, entry_weight, mix_weight, pool_gain, back_weight)
        bf16 = jnp.bfloat16
        dma = pltpu.SemaphoreType.DMA
        flow = pltpu.VMEM((layers, n_s, half, cols), bf16)
        vmem = pl.BlockSpec(memory_space=pltpu.VMEM)
        return pl.pallas_call(
            functools.partial(kernel, (n_g, n_s, n_t)),
            out_shape=jax.ShapeDtypeStruct((rows, channels), bf16),
            in_specs=[vmem] * 6,
            out_specs=vmem,
            scratch_shapes=[
                pltpu.VMEM((layers, n_s * depth, width), bf16),
                pltpu.VMEM((layers, n_s, back_weight.shape[1], cols), bf16),
                pltpu.VMEM((n_s, rows, cols), bf16),
                pltpu.VMEM((rows, channels), bf16),
                pltpu.VMEM((layers, rows + 2 * HALO, width), bf16),
                pltpu.VMEM((rows, width), bf16),
                pltpu.VMEM((half, cols), bf16),
                flow, flow, flow, flow,
                dma((2 * layers, n_s, SUBS, 2)),
                dma((2 * layers, n_s, SUBS)),
                dma((2 * layers, n_s, SUBS)),
                dma((2 * layers, n_s, SUBS)),
                dma((layers, 2)),
                dma((layers, 2)),
                dma((layers, n_s)),
                dma((layers, n_s)),
                dma((layers, n_s)),
                dma((layers, n_s)),
                dma((layers, n_s)),
                dma((layers, n_s)),
                dma((2 * layers,)),
            ],
            compiler_params=pltpu.CompilerParams(
                collective_id=0, has_side_effects=True, vmem_limit_bytes=56 * 1024 * 1024
            ),
        )(tokens, norm_gain, entry_weight, mix_weight, pool_gain, back_weight)

    return jax.shard_map(
        per_device,
        mesh=mesh,
        in_specs=(
            P(("grp", "sp"), None),
            P(),
            P(None, "sp", "tp"),
            P(None, "tp", None, None),
            P(None, "tp"),
            P(None, "tp", "sp"),
        ),
        out_specs=P(("grp", "sp"), None),
        check_vma=False,
    )
```

```python
import functools

import jax
import jax.numpy as jnp
from jax import lax
from jax.experimental import pallas as pl
from jax.experimental.pallas import tpu as pltpu
from jax.sharding import PartitionSpec as P

EPSILON = 1e-05
MESH = pl.DeviceIdType.MESH
LANES = 128
GROUPS = 4
LAYERS = 2
HALO = 16
SUBS = 2


def kernel(
    sizes,
    tok_ref, gain_ref, entry_ref, mix_hbm, pgain_ref, back_ref,
    out_ref,
    mix_ref, went, wback, state, normed, ext, mixed, t_own, t_out, t_in, s_own, s_in,
    zsend, zrecv, ysend, yrecv, hsend, hrecv, asend, arecv, bsend, brecv, csend, crecv, lsem, osem,
):
    n_g, n_s, n_t = sizes
    layers, depth, width = entry_ref.shape
    rows, channels = tok_ref.shape
    cols = back_ref.shape[2]
    half = rows // 2
    pairs = 2 if n_g % 2 == 0 else 1
    g, s, t = lax.axis_index("grp"), lax.axis_index("sp"), lax.axis_index("tp")
    h = lax.rem(g, pairs)
    y_dev = {"grp": g + 1 - 2 * h}
    core = lax.rem(t, 2)
    chip = lax.rem(t // 2, 2)
    core_dev = {"tp": t + 1 - 2 * core}
    x_dev = {"tp": t + 2 - 4 * chip}
    right, left = {"sp": s + 1}, {"sp": s - 1}
    has_right, has_left = s < n_s - 1, s > 0

    barrier = pltpu.get_barrier_semaphore()

    def greet(device):
        pl.semaphore_signal(barrier, inc=1, device_id=device, device_id_type=MESH)

    greet(core_dev)
    greet(x_dev)
    if pairs == 2:
        greet(y_dev)
    pl.when(has_right)(lambda: greet(right))
    pl.when(has_left)(lambda: greet(left))
    pl.semaphore_wait(
        barrier, 1 + pairs + has_right.astype(jnp.int32) + has_left.astype(jnp.int32)
    )

    block_rows = (depth, back_ref.shape[1])

    def piece(m, o, part, c):
        layer, which = divmod(m, 2)
        size = block_rows[which] // (pairs * SUBS)
        start = pl.multiple_of((part * SUBS + c) * size, size)
        if which == 0:
            return went.at[layer, pl.ds(pl.multiple_of(o * depth + start, size), size)]
        return wback.at[layer, o, pl.ds(start, size)]

    def own_piece(m, c):
        layer, which = divmod(m, 2)
        size = block_rows[which] // (pairs * SUBS)
        ref = (entry_ref, back_ref)[which]
        return ref.at[layer, pl.ds(pl.multiple_of((h * SUBS + c) * size, size), size)]

    def z_copy(m, o, c, to_right, own=False):
        return pltpu.make_async_remote_copy(
            src_ref=own_piece(m, c) if own else piece(m, o, h, c),
            dst_ref=piece(m, o, h, c),
            send_sem=zsend.at[m, o, c, 0 if to_right else 1],
            recv_sem=zrecv.at[m, o, c],
            device_id=right if to_right else left,
            device_id_type=MESH,
        )

    def y_copy(m, o, c, part):
        return pltpu.make_async_remote_copy(
            src_ref=piece(m, o, part, c),
            dst_ref=piece(m, o, part, c),
            send_sem=ysend.at[m, o, c],
            recv_sem=yrecv.at[m, o, c],
            device_id=y_dev,
            device_id_type=MESH,
        )

    def send_own(m):
        for c in range(SUBS):
            pl.when(has_right)(lambda: z_copy(m, s, c, True, own=True).start())
            pl.when(has_left)(lambda: z_copy(m, s, c, False, own=True).start())

    def sides(d):
        return ((s >= d, s - d, True, has_right), (s + d < n_s, s + d, False, has_left))

    def forward(m, d):
        for c in range(SUBS):
            for there, o, to_right, onward in sides(d):
                @pl.when(there)
                def _():
                    z_copy(m, o, c, to_right).wait_recv()
                    pl.when(onward)(lambda: z_copy(m, o, c, to_right).start())
                    if pairs == 2:
                        y_copy(m, o, c, h).start()

    def await_y(m, o):
        if pairs == 2:
            for c in range(SUBS):
                y_copy(m, o, c, 1 - h).wait_recv()

    def await_y_all(m):
        for d in range(1, n_s):
            for there, o, _, _ in sides(d):
                pl.when(there)(lambda: await_y(m, o))

    send_own(0)

    locals_ = [pltpu.make_async_copy(mix_hbm, mix_ref, lsem.at[0])]
    for layer in range(layers):
        own = went.at[layer, pl.ds(pl.multiple_of(s * depth, depth), depth)]
        locals_.append(pltpu.make_async_copy(entry_ref.at[layer], own, lsem.at[2 * layer + 1]))
        own = wback.at[layer, s]
        locals_.append(pltpu.make_async_copy(back_ref.at[layer], own, lsem.at[2 * layer + 2]))
    tokens_in = [
        pltpu.make_async_copy(
            tok_ref.at[:, pl.ds(o * cols, cols)], state.at[o], lsem.at[2 * layers + 1 + o]
        )
        for o in range(n_s)
    ]
    for copy in tokens_in + locals_:
        copy.start()

    def normalize(layer):
        def body(i, carry):
            at = pl.ds(pl.multiple_of(i * 32, 32), 32)
            total = jnp.zeros((32, 1), jnp.float32)
            for o in range(n_s):
                value = state[o, at, :].astype(jnp.float32)
                total = total + jnp.sum(value * value, axis=-1, keepdims=True)
            scale = lax.rsqrt(total / channels + EPSILON)
            for o in range(n_s):
                value = state[o, at, :].astype(jnp.float32)
                gain = gain_ref[layer:layer + 1, o * cols:(o + 1) * cols]
                normed[at, o * cols:(o + 1) * cols] = (value * scale * gain).astype(jnp.bfloat16)
            return carry

        lax.fori_loop(0, rows // 32, body, 0)

    def halo_copy(layer, to_right):
        src = rows - HALO if to_right else 0
        dst = rows if to_right else rows + HALO
        side = 0 if to_right else 1
        return pltpu.make_async_remote_copy(
            src_ref=ext.at[layer, pl.ds(src, HALO)],
            dst_ref=ext.at[layer, pl.ds(dst, HALO)],
            send_sem=hsend.at[layer, side],
            recv_sem=hrecv.at[layer, side],
            device_id=right if to_right else left,
            device_id_type=MESH,
        )

    def entry(layer):
        ext[layer, 0:rows] = jnp.dot(
            normed[...], went[layer], preferred_element_type=jnp.float32
        ).astype(jnp.bfloat16)
        pl.when(has_right)(lambda: halo_copy(layer, True).start())
        pl.when(has_left)(lambda: halo_copy(layer, False).start())
        zero = jnp.zeros((HALO, width), jnp.bfloat16)

        @pl.when(s == 0)
        def _():
            ext[layer, rows:rows + HALO] = zero

        @pl.when(s == n_s - 1)
        def _():
            ext[layer, rows + HALO:rows + 2 * HALO] = zero

    def pool(layer):
        pl.when(has_left)(lambda: halo_copy(layer, True).wait_recv())
        pl.when(has_right)(lambda: halo_copy(layer, False).wait_recv())
        reach = jnp.left_shift(jnp.int32(1), t)
        shape = (rows, rows + 2 * HALO)
        row = lax.broadcasted_iota(jnp.int32, shape, 0)
        j = lax.broadcasted_iota(jnp.int32, shape, 1)
        position = jnp.where(j < rows, j, jnp.where(j < rows + HALO, j - rows - HALO, j - HALO))
        offset = position - row
        band = jnp.where((offset >= -reach) & (offset < reach), 1.0, 0.0).astype(jnp.bfloat16)
        summed = jnp.dot(band, ext[layer], preferred_element_type=jnp.float32)
        at = s * rows + lax.broadcasted_iota(jnp.int32, (rows, 1), 0)
        counted = jnp.minimum(at + reach, n_s * rows) - jnp.maximum(at - reach, 0)
        means = summed / counted.astype(jnp.float32)
        differ = (means - ext[layer, 0:rows].astype(jnp.float32)).astype(jnp.bfloat16)
        product = jnp.dot(differ, mix_ref[layer, 0], preferred_element_type=jnp.float32)
        mixed[...] = (product * pgain_ref[layer:layer + 1, :]).astype(jnp.bfloat16)

    keep = pl.ds(pl.multiple_of(core * half, half), half)
    give = pl.ds(pl.multiple_of((1 - core) * half, half), half)
    turn = 1 - 2 * (s // ((n_s + 1) // 2))

    def block_of(k):
        return lax.rem(s + turn * k + n_s, n_s)

    def a_copy(layer, k):
        return pltpu.make_async_remote_copy(
            src_ref=t_out.at[layer, k], dst_ref=t_in.at[layer, k],
            send_sem=asend.at[layer, k], recv_sem=arecv.at[layer, k],
            device_id=core_dev, device_id_type=MESH,
        )

    def b_copy(layer, k):
        return pltpu.make_async_remote_copy(
            src_ref=s_own.at[layer, k], dst_ref=s_in.at[layer, k],
            send_sem=bsend.at[layer, k], recv_sem=brecv.at[layer, k],
            device_id=x_dev, device_id_type=MESH,
        )

    def c_copy(layer, k, rows_at):
        o = block_of(k)
        return pltpu.make_async_remote_copy(
            src_ref=state.at[o, rows_at], dst_ref=state.at[o, rows_at],
            send_sem=csend.at[layer, k], recv_sem=crecv.at[layer, k],
            device_id=core_dev, device_id_type=MESH,
        )

    def back(layer, k):
        o = block_of(k)
        if k > 0:
            await_y(2 * layer + 1, o)
        weight = wback[layer, o]
        t_out[layer, k] = jnp.dot(
            mixed[give, :], weight, preferred_element_type=jnp.float32
        ).astype(jnp.bfloat16)
        a_copy(layer, k).start()
        t_own[layer, k] = jnp.dot(
            mixed[keep, :], weight, preferred_element_type=jnp.float32
        ).astype(jnp.bfloat16)

    def join(layer, k):
        a_copy(layer, k).wait_recv()
        s_own[layer, k] = (
            t_own[layer, k].astype(jnp.float32) + t_in[layer, k].astype(jnp.float32)
        ).astype(jnp.bfloat16)
        b_copy(layer, k).start()

    def finish(layer, k):
        o = block_of(k)
        b_copy(layer, k).wait_recv()
        state[o, keep] = (
            state[o, keep].astype(jnp.float32)
            + (s_own[layer, k].astype(jnp.float32) + s_in[layer, k].astype(jnp.float32))
        ).astype(jnp.bfloat16)
        c_copy(layer, k, keep).start()

    def out_copy(k):
        o = block_of(k)
        return pltpu.make_async_copy(
            state.at[o],
            out_ref.at[:, pl.ds(pl.multiple_of(o * cols, cols), cols)],
            osem.at[k],
        )

    def settle(layer):
        for k in range(n_s):
            c_copy(layer, k, give).wait_recv()
            if layer == layers - 1:
                out_copy(k).start()
            c_copy(layer, k, keep).wait_send()

    early = max(1, n_s - 2)

    def gather(m, first, last):
        for d in range(first, last):
            forward(m, d)
            if d == early and m + 1 < 2 * layers:
                send_own(m + 1)

    for copy in tokens_in:
        copy.wait()
    normalize(0)
    gather(0, 1, n_s)
    for layer in range(layers):
        m = 2 * layer
        last = layer == layers - 1
        gather(m + 1, 1, 2)
        if layer == 0:
            for copy in locals_:
                copy.wait()
        await_y_all(m)
        entry(layer)
        gather(m + 1, 2, early + 1)
        pool(layer)
        for k in range(n_s):
            if k == min(2, n_s - 1):
                gather(m + 1, early + 1, n_s)
                if not last:
                    gather(m + 2, 1, 2)
            back(layer, k)
            if k > 0:
                join(layer, k - 1)
        join(layer, n_s - 1)
        if not last:
            gather(m + 2, 2, early + 1)
        for k in range(n_s):
            finish(layer, k)
        if not last:
            gather(m + 2, early + 1, n_s)
        settle(layer)
        if not last:
            normalize(layer + 1)

    for k in range(n_s):
        out_copy(k).wait()

    for layer in range(layers):
        pl.when(has_right)(lambda: halo_copy(layer, True).wait_send())
        pl.when(has_left)(lambda: halo_copy(layer, False).wait_send())
        for k in range(n_s):
            a_copy(layer, k).wait_send()
            b_copy(layer, k).wait_send()
    for m in range(2 * layers):
        for c in range(SUBS):
            pl.when(has_right)(lambda: z_copy(m, s, c, True, own=True).wait_send())
            pl.when(has_left)(lambda: z_copy(m, s, c, False, own=True).wait_send())
            for d in range(1, n_s):
                for there, o, to_right, onward in sides(d):
                    @pl.when(there)
                    def _():
                        pl.when(onward)(lambda: z_copy(m, o, c, to_right).wait_send())
                        if pairs == 2:
                            y_copy(m, o, c, h).wait_send()


def extended_2(value, sides, width):
    for axis, dim in sides:
        size, length = (lax.axis_size(axis), value.shape[dim])
        up = [(i, (i + 1) % size) for i in range(size - 1)]
        down = [(j, i) for i, j in up]
        last = lax.slice_in_dim(value, length - width, length, axis=dim)
        first = lax.slice_in_dim(value, 0, width, axis=dim)
        before = lax.ppermute(last, axis, up)
        after = lax.ppermute(first, axis, down)
        value = jnp.concatenate([before, value, after], axis=dim)
    return value


def window_mean(padded, positions, halves, total_length, reach):
    row_count = positions.shape[0]
    summed = jnp.zeros((row_count,) + padded.shape[1:], jnp.float32)
    for offset in range(-reach, reach):
        inside = ((offset >= -halves) & (offset < halves)).astype(jnp.float32)
        summed = (
            summed + padded[reach + offset : reach + offset + row_count] * inside[None, :, None]
        )
    lower = jnp.maximum(positions[:, None] - halves[None, :], 0)
    upper = jnp.minimum(positions[:, None] + halves[None, :], total_length)
    counted = (upper - lower).astype(jnp.float32)
    return summed / counted[:, :, None]


def normalize(state, gain):
    values = state.astype(jnp.float32)
    scaled = values * lax.rsqrt(jnp.mean(values * values, axis=-1, keepdims=True) + EPSILON)
    return (scaled * gain).astype(jnp.bfloat16)


def pool_groups(pooled_in, mix_layer, gain_layer, reach):
    row_count = pooled_in.shape[0]
    group_here = mix_layer.shape[0]
    width = mix_layer.shape[1]
    extended = extended_2(pooled_in, (("sp", 0),), reach)
    first_group = lax.axis_index("tp") * group_here
    halves = jnp.left_shift(jnp.int32(1), first_group + jnp.arange(group_here, dtype=jnp.int32))
    positions = lax.axis_index("sp") * row_count + jnp.arange(row_count, dtype=jnp.int32)
    total_length = lax.axis_size("sp") * row_count
    padded = extended.reshape(row_count + 2 * reach, group_here, width).astype(jnp.float32)
    means = window_mean(padded, positions, halves, total_length, reach)
    differ = (means - padded[reach : reach + row_count]).astype(jnp.bfloat16)
    mixed = jnp.einsum("tgc,gcd->tgd", differ, mix_layer, preferred_element_type=jnp.float32)
    return (mixed.reshape(row_count, group_here * width) * gain_layer).astype(jnp.bfloat16)


def plain(tokens, norm_gain, entry_weight, mix_weight, pool_gain, back_weight):
    reach = 2 ** (GROUPS - 1)
    state = tokens
    entry_all, back_all = (
        lax.all_gather(entry_weight, "sp", axis=1, tiled=True),
        lax.all_gather(back_weight, "sp", axis=2, tiled=True),
    )
    for layer in range(LAYERS):
        normed = normalize(state, norm_gain[layer])
        pooled_in = jnp.dot(normed, entry_all[layer], preferred_element_type=jnp.float32).astype(
            jnp.bfloat16
        )
        back_local = back_all[layer]
        mixed = pool_groups(pooled_in, mix_weight[layer], pool_gain[layer], reach)
        update = jnp.dot(mixed, back_local, preferred_element_type=jnp.float32)
        summed = lax.psum(update.astype(jnp.bfloat16), "tp").astype(jnp.float32)
        state = (state.astype(jnp.float32) + summed).astype(jnp.bfloat16)
    return state


def solution(mesh):
    n_g, n_s, n_t = mesh.shape["grp"], mesh.shape["sp"], mesh.shape["tp"]

    def per_device(tokens, norm_gain, entry_weight, mix_weight, pool_gain, back_weight):
        layers, depth, width = entry_weight.shape
        rows, channels = tokens.shape
        cols = back_weight.shape[2]
        half = rows // 2
        if n_t != 4 or cols % LANES or depth % LANES or rows % (2 * HALO):
            return plain(tokens, norm_gain, entry_weight, mix_weight, pool_gain, back_weight)
        bf16 = jnp.bfloat16
        dma = pltpu.SemaphoreType.DMA
        flow = pltpu.VMEM((layers, n_s, half, cols), bf16)
        vmem = pl.BlockSpec(memory_space=pltpu.VMEM)
        hbm = pl.BlockSpec(memory_space=pl.ANY)
        return pl.pallas_call(
            functools.partial(kernel, (n_g, n_s, n_t)),
            out_shape=jax.ShapeDtypeStruct((rows, channels), bf16),
            in_specs=[hbm, vmem, hbm, hbm, vmem, hbm],
            out_specs=hbm,
            scratch_shapes=[
                pltpu.VMEM(mix_weight.shape, bf16),
                pltpu.VMEM((layers, n_s * depth, width), bf16),
                pltpu.VMEM((layers, n_s, back_weight.shape[1], cols), bf16),
                pltpu.VMEM((n_s, rows, cols), bf16),
                pltpu.VMEM((rows, channels), bf16),
                pltpu.VMEM((layers, rows + 2 * HALO, width), bf16),
                pltpu.VMEM((rows, width), bf16),
                flow, flow, flow, flow, flow,
                dma((2 * layers, n_s, SUBS, 2)),
                dma((2 * layers, n_s, SUBS)),
                dma((2 * layers, n_s, SUBS)),
                dma((2 * layers, n_s, SUBS)),
                dma((layers, 2)),
                dma((layers, 2)),
                dma((layers, n_s)),
                dma((layers, n_s)),
                dma((layers, n_s)),
                dma((layers, n_s)),
                dma((layers, n_s)),
                dma((layers, n_s)),
                dma((2 * layers + 1 + n_s,)),
                dma((n_s,)),
            ],
            compiler_params=pltpu.CompilerParams(
                collective_id=0, has_side_effects=True, vmem_limit_bytes=56 * 1024 * 1024
            ),
        )(tokens, norm_gain, entry_weight, mix_weight, pool_gain, back_weight)

    return jax.shard_map(
        per_device,
        mesh=mesh,
        in_specs=(
            P(("grp", "sp"), None),
            P(),
            P(None, "sp", "tp"),
            P(None, "tp", None, None),
            P(None, "tp"),
            P(None, "tp", "sp"),
        ),
        out_specs=P(("grp", "sp"), None),
        check_vma=False,
    )
```

```python
import functools

import jax
import jax.numpy as jnp
from jax import lax
from jax.experimental import pallas as pl
from jax.experimental.pallas import tpu as pltpu
from jax.sharding import PartitionSpec as P

EPSILON = 1e-05
MESH = pl.DeviceIdType.MESH
LANES = 128
GROUPS = 4
LAYERS = 2
HALO = 16
SUBS = 2


def kernel(
    sizes,
    tok_ref, gain_ref, entry_ref, mix_hbm, pgain_ref, back_ref,
    out_ref,
    mix_ref, went, wback, state, normed, ext, mixed, t_own, t_out, t_in, s_own, s_in,
    zsend, zrecv, ysend, yrecv, hsend, hrecv, asend, arecv, bsend, brecv, csend, crecv, lsem, osem,
):
    n_g, n_s, n_t = sizes
    layers, depth, width = entry_ref.shape
    rows, channels = tok_ref.shape
    cols = back_ref.shape[2]
    half = rows // 2
    pairs = 2 if n_g % 2 == 0 else 1
    g, s, t = lax.axis_index("grp"), lax.axis_index("sp"), lax.axis_index("tp")
    h = lax.rem(g, pairs)
    y_dev = {"grp": g + 1 - 2 * h}
    core = lax.rem(t, 2)
    chip = lax.rem(t // 2, 2)
    core_dev = {"tp": t + 1 - 2 * core}
    x_dev = {"tp": t + 2 - 4 * chip}
    right, left = {"sp": s + 1}, {"sp": s - 1}
    has_right, has_left = s < n_s - 1, s > 0

    barrier = pltpu.get_barrier_semaphore()

    def greet(device):
        pl.semaphore_signal(barrier, inc=1, device_id=device, device_id_type=MESH)

    greet(core_dev)
    greet(x_dev)
    if pairs == 2:
        greet(y_dev)
    pl.when(has_right)(lambda: greet(right))
    pl.when(has_left)(lambda: greet(left))
    pl.semaphore_wait(
        barrier, 1 + pairs + has_right.astype(jnp.int32) + has_left.astype(jnp.int32)
    )

    block_rows = (depth, back_ref.shape[1])

    def piece(m, o, part, c):
        layer, which = divmod(m, 2)
        size = block_rows[which] // (pairs * SUBS)
        start = pl.multiple_of((part * SUBS + c) * size, size)
        if which == 0:
            return went.at[layer, pl.ds(pl.multiple_of(o * depth + start, size), size)]
        return wback.at[layer, o, pl.ds(start, size)]

    def own_piece(m, c):
        layer, which = divmod(m, 2)
        size = block_rows[which] // (pairs * SUBS)
        ref = (entry_ref, back_ref)[which]
        return ref.at[layer, pl.ds(pl.multiple_of((h * SUBS + c) * size, size), size)]

    def z_copy(m, o, c, to_right, own=False):
        return pltpu.make_async_remote_copy(
            src_ref=own_piece(m, c) if own else piece(m, o, h, c),
            dst_ref=piece(m, o, h, c),
            send_sem=zsend.at[m, o, c, 0 if to_right else 1],
            recv_sem=zrecv.at[m, o, c],
            device_id=right if to_right else left,
            device_id_type=MESH,
        )

    def y_copy(m, o, c, part):
        return pltpu.make_async_remote_copy(
            src_ref=piece(m, o, part, c),
            dst_ref=piece(m, o, part, c),
            send_sem=ysend.at[m, o, c],
            recv_sem=yrecv.at[m, o, c],
            device_id=y_dev,
            device_id_type=MESH,
        )

    def send_own(m):
        for c in range(SUBS):
            pl.when(has_right)(lambda: z_copy(m, s, c, True, own=True).start())
            pl.when(has_left)(lambda: z_copy(m, s, c, False, own=True).start())

    def sides(d):
        return ((s >= d, s - d, True, has_right), (s + d < n_s, s + d, False, has_left))

    def forward(m, d):
        for c in range(SUBS):
            for there, o, to_right, onward in sides(d):
                @pl.when(there)
                def _():
                    z_copy(m, o, c, to_right).wait_recv()
                    pl.when(onward)(lambda: z_copy(m, o, c, to_right).start())
                    if pairs == 2:
                        y_copy(m, o, c, h).start()

    def await_y(m, o):
        if pairs == 2:
            for c in range(SUBS):
                y_copy(m, o, c, 1 - h).wait_recv()

    def await_y_all(m):
        for d in range(1, n_s):
            for there, o, _, _ in sides(d):
                pl.when(there)(lambda: await_y(m, o))

    send_own(0)

    locals_ = [pltpu.make_async_copy(mix_hbm, mix_ref, lsem.at[0])]
    for layer in range(layers):
        own = went.at[layer, pl.ds(pl.multiple_of(s * depth, depth), depth)]
        locals_.append(pltpu.make_async_copy(entry_ref.at[layer], own, lsem.at[2 * layer + 1]))
        own = wback.at[layer, s]
        locals_.append(pltpu.make_async_copy(back_ref.at[layer], own, lsem.at[2 * layer + 2]))
    tokens_in = [
        pltpu.make_async_copy(
            tok_ref.at[:, pl.ds(o * cols, cols)], state.at[o], lsem.at[2 * layers + 1 + o]
        )
        for o in range(n_s)
    ]
    for copy in tokens_in + locals_:
        copy.start()

    def normalize(layer):
        def body(i, carry):
            at = pl.ds(pl.multiple_of(i * 32, 32), 32)
            total = jnp.zeros((32, 1), jnp.float32)
            for o in range(n_s):
                value = state[o, at, :].astype(jnp.float32)
                total = total + jnp.sum(value * value, axis=-1, keepdims=True)
            scale = lax.rsqrt(total / channels + EPSILON)
            for o in range(n_s):
                value = state[o, at, :].astype(jnp.float32)
                gain = gain_ref[layer:layer + 1, o * cols:(o + 1) * cols]
                normed[at, o * cols:(o + 1) * cols] = (value * scale * gain).astype(jnp.bfloat16)
            return carry

        lax.fori_loop(0, rows // 32, body, 0)

    def halo_copy(layer, to_right):
        src = rows - HALO if to_right else 0
        dst = rows if to_right else rows + HALO
        side = 0 if to_right else 1
        return pltpu.make_async_remote_copy(
            src_ref=ext.at[layer, pl.ds(src, HALO)],
            dst_ref=ext.at[layer, pl.ds(dst, HALO)],
            send_sem=hsend.at[layer, side],
            recv_sem=hrecv.at[layer, side],
            device_id=right if to_right else left,
            device_id_type=MESH,
        )

    def entry(layer):
        ext[layer, 0:rows] = jnp.dot(
            normed[...], went[layer], preferred_element_type=jnp.float32
        ).astype(jnp.bfloat16)
        pl.when(has_right)(lambda: halo_copy(layer, True).start())
        pl.when(has_left)(lambda: halo_copy(layer, False).start())
        zero = jnp.zeros((HALO, width), jnp.bfloat16)

        @pl.when(s == 0)
        def _():
            ext[layer, rows:rows + HALO] = zero

        @pl.when(s == n_s - 1)
        def _():
            ext[layer, rows + HALO:rows + 2 * HALO] = zero

    def pool(layer):
        pl.when(has_left)(lambda: halo_copy(layer, True).wait_recv())
        pl.when(has_right)(lambda: halo_copy(layer, False).wait_recv())
        reach = jnp.left_shift(jnp.int32(1), t)
        shape = (rows, rows + 2 * HALO)
        row = lax.broadcasted_iota(jnp.int32, shape, 0)
        j = lax.broadcasted_iota(jnp.int32, shape, 1)
        position = jnp.where(j < rows, j, jnp.where(j < rows + HALO, j - rows - HALO, j - HALO))
        offset = position - row
        band = jnp.where((offset >= -reach) & (offset < reach), 1.0, 0.0).astype(jnp.bfloat16)
        summed = jnp.dot(band, ext[layer], preferred_element_type=jnp.float32)
        at = s * rows + lax.broadcasted_iota(jnp.int32, (rows, 1), 0)
        counted = jnp.minimum(at + reach, n_s * rows) - jnp.maximum(at - reach, 0)
        means = summed / counted.astype(jnp.float32)
        differ = (means - ext[layer, 0:rows].astype(jnp.float32)).astype(jnp.bfloat16)
        product = jnp.dot(differ, mix_ref[layer, 0], preferred_element_type=jnp.float32)
        mixed[...] = (product * pgain_ref[layer:layer + 1, :]).astype(jnp.bfloat16)

    keep = pl.ds(pl.multiple_of(core * half, half), half)
    give = pl.ds(pl.multiple_of((1 - core) * half, half), half)
    turn = 1 - 2 * (s // ((n_s + 1) // 2))

    def block_of(k):
        return lax.rem(s + turn * k + n_s, n_s)

    def a_copy(layer, k):
        return pltpu.make_async_remote_copy(
            src_ref=t_out.at[layer, k], dst_ref=t_in.at[layer, k],
            send_sem=asend.at[layer, k], recv_sem=arecv.at[layer, k],
            device_id=core_dev, device_id_type=MESH,
        )

    def b_copy(layer, k):
        return pltpu.make_async_remote_copy(
            src_ref=s_own.at[layer, k], dst_ref=s_in.at[layer, k],
            send_sem=bsend.at[layer, k], recv_sem=brecv.at[layer, k],
            device_id=x_dev, device_id_type=MESH,
        )

    def c_copy(layer, k, rows_at):
        o = block_of(k)
        return pltpu.make_async_remote_copy(
            src_ref=state.at[o, rows_at], dst_ref=state.at[o, rows_at],
            send_sem=csend.at[layer, k], recv_sem=crecv.at[layer, k],
            device_id=core_dev, device_id_type=MESH,
        )

    def back(layer, k):
        o = block_of(k)
        if k > 0:
            await_y(2 * layer + 1, o)
        weight = wback[layer, o]
        t_out[layer, k] = jnp.dot(
            mixed[give, :], weight, preferred_element_type=jnp.float32
        ).astype(jnp.bfloat16)
        a_copy(layer, k).start()
        t_own[layer, k] = jnp.dot(
            mixed[keep, :], weight, preferred_element_type=jnp.float32
        ).astype(jnp.bfloat16)

    def join(layer, k):
        a_copy(layer, k).wait_recv()
        s_own[layer, k] = (
            t_own[layer, k].astype(jnp.float32) + t_in[layer, k].astype(jnp.float32)
        ).astype(jnp.bfloat16)
        b_copy(layer, k).start()

    def finish(layer, k):
        o = block_of(k)
        b_copy(layer, k).wait_recv()
        state[o, keep] = (
            state[o, keep].astype(jnp.float32)
            + (s_own[layer, k].astype(jnp.float32) + s_in[layer, k].astype(jnp.float32))
        ).astype(jnp.bfloat16)
        c_copy(layer, k, keep).start()

    def out_copy(k):
        o = block_of(k)
        return pltpu.make_async_copy(
            state.at[o],
            out_ref.at[:, pl.ds(pl.multiple_of(o * cols, cols), cols)],
            osem.at[k],
        )

    def settle(layer):
        for k in range(n_s):
            c_copy(layer, k, give).wait_recv()
            if layer == layers - 1:
                out_copy(k).start()
            c_copy(layer, k, keep).wait_send()

    early = max(1, n_s - 2)

    def gather(m, first, last):
        for d in range(first, last):
            forward(m, d)
            if d == early and m + 1 < 2 * layers:
                send_own(m + 1)

    for copy in tokens_in:
        copy.wait()
    normalize(0)
    gather(0, 1, n_s)
    for layer in range(layers):
        m = 2 * layer
        last = layer == layers - 1
        gather(m + 1, 1, 2)
        if layer == 0:
            for copy in locals_:
                copy.wait()
        await_y_all(m)
        entry(layer)
        gather(m + 1, 2, early + 1)
        pool(layer)
        for k in range(n_s):
            if k == min(2, n_s - 1):
                gather(m + 1, early + 1, n_s)
                if not last:
                    gather(m + 2, 1, 2)
            back(layer, k)
            if k > 0:
                join(layer, k - 1)
        join(layer, n_s - 1)
        if not last:
            gather(m + 2, 2, n_s)
        for k in range(n_s):
            finish(layer, k)
        settle(layer)
        if not last:
            normalize(layer + 1)

    for k in range(n_s):
        out_copy(k).wait()

    for layer in range(layers):
        pl.when(has_right)(lambda: halo_copy(layer, True).wait_send())
        pl.when(has_left)(lambda: halo_copy(layer, False).wait_send())
        for k in range(n_s):
            a_copy(layer, k).wait_send()
            b_copy(layer, k).wait_send()
    for m in range(2 * layers):
        for c in range(SUBS):
            pl.when(has_right)(lambda: z_copy(m, s, c, True, own=True).wait_send())
            pl.when(has_left)(lambda: z_copy(m, s, c, False, own=True).wait_send())
            for d in range(1, n_s):
                for there, o, to_right, onward in sides(d):
                    @pl.when(there)
                    def _():
                        pl.when(onward)(lambda: z_copy(m, o, c, to_right).wait_send())
                        if pairs == 2:
                            y_copy(m, o, c, h).wait_send()


def extended_2(value, sides, width):
    for axis, dim in sides:
        size, length = (lax.axis_size(axis), value.shape[dim])
        up = [(i, (i + 1) % size) for i in range(size - 1)]
        down = [(j, i) for i, j in up]
        last = lax.slice_in_dim(value, length - width, length, axis=dim)
        first = lax.slice_in_dim(value, 0, width, axis=dim)
        before = lax.ppermute(last, axis, up)
        after = lax.ppermute(first, axis, down)
        value = jnp.concatenate([before, value, after], axis=dim)
    return value


def window_mean(padded, positions, halves, total_length, reach):
    row_count = positions.shape[0]
    summed = jnp.zeros((row_count,) + padded.shape[1:], jnp.float32)
    for offset in range(-reach, reach):
        inside = ((offset >= -halves) & (offset < halves)).astype(jnp.float32)
        summed = (
            summed + padded[reach + offset : reach + offset + row_count] * inside[None, :, None]
        )
    lower = jnp.maximum(positions[:, None] - halves[None, :], 0)
    upper = jnp.minimum(positions[:, None] + halves[None, :], total_length)
    counted = (upper - lower).astype(jnp.float32)
    return summed / counted[:, :, None]


def normalize(state, gain):
    values = state.astype(jnp.float32)
    scaled = values * lax.rsqrt(jnp.mean(values * values, axis=-1, keepdims=True) + EPSILON)
    return (scaled * gain).astype(jnp.bfloat16)


def pool_groups(pooled_in, mix_layer, gain_layer, reach):
    row_count = pooled_in.shape[0]
    group_here = mix_layer.shape[0]
    width = mix_layer.shape[1]
    extended = extended_2(pooled_in, (("sp", 0),), reach)
    first_group = lax.axis_index("tp") * group_here
    halves = jnp.left_shift(jnp.int32(1), first_group + jnp.arange(group_here, dtype=jnp.int32))
    positions = lax.axis_index("sp") * row_count + jnp.arange(row_count, dtype=jnp.int32)
    total_length = lax.axis_size("sp") * row_count
    padded = extended.reshape(row_count + 2 * reach, group_here, width).astype(jnp.float32)
    means = window_mean(padded, positions, halves, total_length, reach)
    differ = (means - padded[reach : reach + row_count]).astype(jnp.bfloat16)
    mixed = jnp.einsum("tgc,gcd->tgd", differ, mix_layer, preferred_element_type=jnp.float32)
    return (mixed.reshape(row_count, group_here * width) * gain_layer).astype(jnp.bfloat16)


def plain(tokens, norm_gain, entry_weight, mix_weight, pool_gain, back_weight):
    reach = 2 ** (GROUPS - 1)
    state = tokens
    entry_all, back_all = (
        lax.all_gather(entry_weight, "sp", axis=1, tiled=True),
        lax.all_gather(back_weight, "sp", axis=2, tiled=True),
    )
    for layer in range(LAYERS):
        normed = normalize(state, norm_gain[layer])
        pooled_in = jnp.dot(normed, entry_all[layer], preferred_element_type=jnp.float32).astype(
            jnp.bfloat16
        )
        back_local = back_all[layer]
        mixed = pool_groups(pooled_in, mix_weight[layer], pool_gain[layer], reach)
        update = jnp.dot(mixed, back_local, preferred_element_type=jnp.float32)
        summed = lax.psum(update.astype(jnp.bfloat16), "tp").astype(jnp.float32)
        state = (state.astype(jnp.float32) + summed).astype(jnp.bfloat16)
    return state


def solution(mesh):
    n_g, n_s, n_t = mesh.shape["grp"], mesh.shape["sp"], mesh.shape["tp"]

    def per_device(tokens, norm_gain, entry_weight, mix_weight, pool_gain, back_weight):
        layers, depth, width = entry_weight.shape
        rows, channels = tokens.shape
        cols = back_weight.shape[2]
        half = rows // 2
        if n_t != 4 or cols % LANES or depth % LANES or rows % (2 * HALO):
            return plain(tokens, norm_gain, entry_weight, mix_weight, pool_gain, back_weight)
        bf16 = jnp.bfloat16
        dma = pltpu.SemaphoreType.DMA
        flow = pltpu.VMEM((layers, n_s, half, cols), bf16)
        vmem = pl.BlockSpec(memory_space=pltpu.VMEM)
        hbm = pl.BlockSpec(memory_space=pl.ANY)
        return pl.pallas_call(
            functools.partial(kernel, (n_g, n_s, n_t)),
            out_shape=jax.ShapeDtypeStruct((rows, channels), bf16),
            in_specs=[hbm, vmem, hbm, hbm, vmem, hbm],
            out_specs=hbm,
            scratch_shapes=[
                pltpu.VMEM(mix_weight.shape, bf16),
                pltpu.VMEM((layers, n_s * depth, width), bf16),
                pltpu.VMEM((layers, n_s, back_weight.shape[1], cols), bf16),
                pltpu.VMEM((n_s, rows, cols), bf16),
                pltpu.VMEM((rows, channels), bf16),
                pltpu.VMEM((layers, rows + 2 * HALO, width), bf16),
                pltpu.VMEM((rows, width), bf16),
                flow, flow, flow, flow, flow,
                dma((2 * layers, n_s, SUBS, 2)),
                dma((2 * layers, n_s, SUBS)),
                dma((2 * layers, n_s, SUBS)),
                dma((2 * layers, n_s, SUBS)),
                dma((layers, 2)),
                dma((layers, 2)),
                dma((layers, n_s)),
                dma((layers, n_s)),
                dma((layers, n_s)),
                dma((layers, n_s)),
                dma((layers, n_s)),
                dma((layers, n_s)),
                dma((2 * layers + 1 + n_s,)),
                dma((n_s,)),
            ],
            compiler_params=pltpu.CompilerParams(
                collective_id=0, has_side_effects=True, vmem_limit_bytes=56 * 1024 * 1024
            ),
        )(tokens, norm_gain, entry_weight, mix_weight, pool_gain, back_weight)

    return jax.shard_map(
        per_device,
        mesh=mesh,
        in_specs=(
            P(("grp", "sp"), None),
            P(),
            P(None, "sp", "tp"),
            P(None, "tp", None, None),
            P(None, "tp"),
            P(None, "tp", "sp"),
        ),
        out_specs=P(("grp", "sp"), None),
        check_vma=False,
    )
```
